32 devices in a mesh: sp: 8 (over z, x), tp: 4 (over y, core).
Axes of the slice: x: 2, y: 2, z: 4, core: 2. Of those that a mesh axis runs over, the one named last changes fastest.
Arguments:
- moe_input: bfloat16 [1024, 2048], P('sp'), may hold values from -6 to 6
- out_grad: bfloat16 [1024, 2048], P('sp'), may hold values from -6 to 6
- routes: int32 [1024, 2], P('sp'), may hold values from 0 to 7, all different within a row; in each aligned block of 128 rows (0 to 127, 128 to 255, ...) at most 40 rows name the same one
- route_weight: float32 [1024, 2], P('sp'), may hold values from 0.2 to 1.2
- w_gate: bfloat16 [8, 2048, 2048], P('sp', None, 'tp'), may hold values from -0.125 to 0.125
- w_up: bfloat16 [8, 2048, 2048], P('sp', None, 'tp'), may hold values from -0.125 to 0.125
- w_down: bfloat16 [8, 2048, 2048], P('sp', 'tp'), may hold values from -0.125 to 0.125
- w_out: bfloat16 [2048, 4096], P(None, 'tp'), may hold values from -0.09375 to 0.09375
- query_heads: bfloat16 [16, 1024, 128], P('tp', 'sp'), may hold values from -6 to 6
- key_heads: bfloat16 [16, 1024, 128], P('tp', 'sp'), may hold values from -6 to 6
- value_heads: bfloat16 [16, 1024, 256], P('tp', 'sp'), may hold values from -6 to 6
- log_decay: float32 [16, 1024], P('tp', 'sp'), may hold values from -0.6 to 0
- state_in: float32 [16, 8, 128, 256], P('tp', 'sp'), may hold values from -4 to 4
Outputs:
- gate_grad: bfloat16 [8, 2048, 2048], P('sp', None, 'tp')
- up_grad: bfloat16 [8, 2048, 2048], P('sp', None, 'tp')
- down_grad: bfloat16 [8, 2048, 2048], P('sp', 'tp')
- out_proj_grad: float32 [2048, 4096], P('sp', 'tp')
- query_gradient: bfloat16 [16, 1024, 128], P('tp', 'sp')
- key_grad: bfloat16 [16, 1024, 128], P('tp', 'sp')
- value_grad: bfloat16 [16, 1024, 256], P('tp', 'sp')
The draws below stay inside these ranges and needn't reach their ends.
Inputs may be any that keep to these rules, and one draw needn't show every extreme that they name: `routes`: each row names 2 different experts; within each aligned block of 128 tokens no expert is named more than 40 times, and exactly 40 times for some expert in some blocks.
All inputs are finite; a program needn't handle non-finite values.
Results may differ from the reference program's by a relative error of at most 0.025.
Values may be sent and summed in bfloat16 or wider, within the bound.
A program may use at most 64 MiB of HBM per device.

```python
import math
import jax
import jax.numpy as jnp
import numpy as np
from jax import lax

D = 2048
FF = 2048
RETENTION_HEADS = 16
DK = 128
DV = 256
TOPK = 2
BLOCK = 64
TOK_DEV = 128
SEQUENCE_TOKENS = 1024
EXPERTS = 8
CAP = 40
N_SP = 8
N_TP = 4


def draw_log_decay(key, part):
    random_subkeys = jax.random.split(jax.random.fold_in(key, 11), 6)
    fast_share = 0.5
    quick_heads = jax.random.uniform(random_subkeys[0], (RETENTION_HEADS,), jnp.float32) < fast_share
    fast_rate = jnp.log(10.0) / jax.random.uniform(random_subkeys[1], (RETENTION_HEADS,), jnp.float32, 30.0, 50.0)
    slow_rate = jax.random.uniform(random_subkeys[2], (RETENTION_HEADS,), jnp.float32, 0.2, 0.5) / SEQUENCE_TOKENS
    head_decay_rate = jnp.where(quick_heads, fast_rate, slow_rate)
    span_total = SEQUENCE_TOKENS // TOK_DEV
    span_factor = jnp.exp(jax.random.uniform(random_subkeys[3], (span_total,), jnp.float32, jnp.log(0.5), jnp.log(2.0)))
    position_weighting = jnp.repeat(span_factor, TOK_DEV)
    surge_locations = jax.random.randint(random_subkeys[4], (RETENTION_HEADS, 2), 0, SEQUENCE_TOKENS)
    surge_depth = jnp.log(jax.random.uniform(random_subkeys[5], (RETENTION_HEADS, 2), jnp.float32, 0.6, 0.8))
    token_positions = jnp.arange(SEQUENCE_TOKENS, dtype=jnp.int32)
    match_flags = token_positions[None, :, None] == surge_locations[:, None, :]
    surge_events = jnp.sum(jnp.where(match_flags, surge_depth[:, None, :], 0.0), axis=2)
    logarithm_values = -head_decay_rate[:, None] * position_weighting[None, :] + jnp.where(quick_heads[:, None], 0.0, surge_events)
    return logarithm_values.astype(jnp.float32)


def spiked(values, own_key, source, target, parts, factor):
    owner, partner = [(jnp.arange(values.shape[position]) // (values.shape[position] // parts)).reshape([-1 if axis == position else 1 for axis in range(values.ndim)]) for position in (source, target)]
    chosen = jax.random.permutation(own_key, parts)[partner]
    strong = (owner == chosen) | (owner == (partner + parts // 2) % parts)
    return jnp.where(strong, factor * values, values)


def block_scale(own_key, shape, shards, least, top_value):
    def one(position, blocks):
        heights = jax.random.uniform(jax.random.fold_in(jax.random.fold_in(own_key, 6), position), (blocks,), jnp.float32, least / len(shards), top_value / len(shards))
        return jnp.repeat(jnp.exp(heights), shape[position] // blocks).reshape((-1,) + (1,) * (len(shape) - position - 1))

    loudness = one(*shards[0])
    for cut in shards[1:]:
        loudness = loudness * one(*cut)
    return loudness


def deal_out(rng, own, number, rows, number_of, top, reach, slope):
    ranking = jax.random.permutation(rng, number_of)
    heavy_load, ordinary = load_shares(number_of, rows * top, reach, slope, True), load_shares(number_of, rows * top, reach, slope, False)
    places = jnp.arange(number_of)

    def named(sizes, offset_by):
        used = int((sizes > 0).sum())
        fixed = max(1, used // 4)
        moved = fixed + (places - fixed + offset_by * (used - fixed)) % max(1, number_of - fixed)
        return jnp.zeros((number_of,), jnp.int32).at[ranking[jnp.where(places < fixed, places, moved)]].set(jnp.asarray(sizes, jnp.int32))

    sizes = jnp.where(number % 4 == 0, named(heavy_load, number // 4), named(ordinary, number - number // 4 - 1))
    mixed = jax.random.permutation(jax.random.fold_in(own, 3), number_of)
    giver, taker = mixed[0:number_of // 2 * 2:2], mixed[1:number_of // 2 * 2:2]
    room = jnp.minimum(sizes[giver] - 1, reach - sizes[taker]) // 2
    room = jnp.where((giver == ranking[0]) | (taker == ranking[0]) | (sizes[taker] == 0), 0, jnp.maximum(room, 0))
    moved = jax.random.randint(jax.random.fold_in(own, 4), (number_of // 2,), 0, 1 << 20) % (room + 1)
    sizes = sizes.at[giver].add(-moved).at[taker].add(moved)
    items = jnp.searchsorted(jnp.cumsum(sizes), jnp.arange(rows * top), side="right").astype(jnp.int32)
    grid = items.reshape(top, rows).T
    grid = grid[jax.random.permutation(jax.random.fold_in(own, 1), rows)]
    offset_by = jax.random.randint(jax.random.fold_in(own, 2), (rows, 1), 0, top)
    return jnp.take_along_axis(grid, (jnp.arange(top)[None, :] + offset_by) % top, axis=1)


def load_shares(amount, total, most, lean, full):
    weights = [(1 << 20) // math.isqrt(rank ** lean) + 1 for rank in range(1, amount + 1)]
    largest = most if full else min(most, max(-(-total // amount), total * weights[0] // sum(weights)))
    least = 1 if total - largest >= amount - 1 else 0
    counts, rest = [largest] + [least] * (amount - 1), total - largest - least * (amount - 1)
    while rest > 0:
        free = [i for i in range(1, amount) if counts[i] < largest] or [i for i in range(1, amount) if counts[i] < most]
        whole, remaining = sum([weights[i] for i in free]), rest
        for i in free:
            extra = min(most - counts[i], max(1, remaining * weights[i] // whole), rest)
            counts[i] = counts[i] + extra
            rest = rest - extra
    return np.array(counts)


def bell_draw(own_key, shape, width, reach, shards=(), kind=jnp.bfloat16):
    entries = width * jax.random.normal(own_key, shape, jnp.float32)
    if shards:
        entries = entries * block_scale(own_key, shape, shards, -0.22, 0.18)
    return jnp.clip(entries, -reach, reach).astype(kind)


def bell_draw_with(stream_key, dims, scale, most, shards, heavy, kind=jnp.bfloat16):
    values = scale * jax.random.normal(stream_key, dims, jnp.float32)
    if shards:
        values = values * block_scale(stream_key, dims, shards, -0.22, 0.18)
    return jnp.clip(spiked(values, jax.random.fold_in(stream_key, 3), *heavy), -most, most).astype(kind)


def setup_inputs(seed: int = 0) -> dict:
    streams_of = jax.random.split(jax.random.key(seed), 14)
    moe_input = bell_draw(streams_of[0], (SEQUENCE_TOKENS, D), 1.0, 6.0, ((0, 8),))
    out_grad = bell_draw_with(streams_of[1], (SEQUENCE_TOKENS, D), 1.0, 6.0, ((0, 8),), (0, 1, 8, 2.0))
    routes_keys = jax.random.split(jax.random.fold_in(streams_of[2], 1), SEQUENCE_TOKENS // TOK_DEV)
    routes_turns = jax.random.permutation(jax.random.fold_in(streams_of[2], 3), SEQUENCE_TOKENS // TOK_DEV)
    routes = jax.vmap(lambda own, number: deal_out(jax.random.fold_in(streams_of[2], 2), own, number, TOK_DEV, EXPERTS, TOPK, CAP, 2))(routes_keys, routes_turns).reshape((SEQUENCE_TOKENS, TOPK))
    route_weight = jnp.clip(0.2 + 1 * jax.random.uniform(streams_of[3], (SEQUENCE_TOKENS, TOPK), jnp.float32) ** block_scale(streams_of[3], (SEQUENCE_TOKENS, TOPK), ((0, 8),), -0.2, 0.2), 0.2, 1.2)
    w_gate = bell_draw(streams_of[4], (EXPERTS, D, FF), D ** -0.5, 0.125, ((0, 8), (2, 4)))
    w_up = bell_draw(streams_of[5], (EXPERTS, D, FF), D ** -0.5, 0.125, ((0, 8), (2, 4)))
    w_down = bell_draw(streams_of[6], (EXPERTS, FF, D), FF ** -0.5, 0.125, ((0, 8), (1, 4)))
    w_out = bell_draw(streams_of[7], (D, RETENTION_HEADS * DV), (RETENTION_HEADS * DV) ** -0.5, 0.09375, ((1, 4),))
    query_heads = bell_draw(streams_of[8], (RETENTION_HEADS, SEQUENCE_TOKENS, DK), 1.0, 6.0, ((0, 4), (1, 8)))
    key_heads = bell_draw(streams_of[9], (RETENTION_HEADS, SEQUENCE_TOKENS, DK), 1.0, 6.0, ((0, 4), (1, 8)))
    value_heads = bell_draw(streams_of[10], (RETENTION_HEADS, SEQUENCE_TOKENS, DV), 1.0, 6.0, ((0, 4), (1, 8)))
    log_decay = draw_log_decay(jax.random.fold_in(streams_of[13], 71), 0)
    state_in = bell_draw(streams_of[12], (RETENTION_HEADS, N_SP, DK, DV), 0.5, 4.0, ((0, 4), (1, 8)), jnp.float32)
    return dict(moe_input=moe_input, out_grad=out_grad, routes=routes, route_weight=route_weight, w_gate=w_gate, w_up=w_up, w_down=w_down, w_out=w_out, query_heads=query_heads, key_heads=key_heads, value_heads=value_heads, log_decay=log_decay, state_in=state_in)


exact_precision = lax.Precision.HIGHEST


def stored(array):
    return lax.optimization_barrier(array.astype(jnp.bfloat16))


def silu_slope(gate_pre):
    sigmoid_v = jax.nn.sigmoid(gate_pre)
    return sigmoid_v * (1.0 + gate_pre * (1.0 - sigmoid_v))


def decay_table(log_sums):
    block_size = log_sums.shape[-1]
    token_positions = jnp.arange(block_size)
    lower_mask = (token_positions[:, None] >= token_positions[None, :])[None]
    log_diff = jnp.where(lower_mask, log_sums[:, :, None] - log_sums[:, None, :], 0.0)
    return jnp.where(lower_mask, jnp.exp(log_diff), 0.0)


def forward_block(forwarded_state, inputs):
    query_rows, rescaled_keys, value_rows, head_gradients, log_sums = inputs
    decay_mat = decay_table(log_sums)
    scores = jnp.einsum('htk,hsk->hts', query_rows, rescaled_keys, precision=exact_precision) * decay_mat
    leading_decay = jnp.exp(log_sums)[:, :, None]
    trailing_decay = jnp.exp(log_sums[:, -1:] - log_sums)[:, :, None]
    blended_heads = jnp.einsum('hts,hsv->htv', scores, value_rows, precision=exact_precision)
    blended_heads = blended_heads + jnp.einsum('imj,iju->imu', query_rows * leading_decay, forwarded_state, precision=exact_precision)
    back_scores = jnp.einsum('htv,hsv->hts', head_gradients, value_rows, precision=exact_precision) * decay_mat
    query_gradient = jnp.einsum('hts,hsk->htk', back_scores, rescaled_keys, precision=exact_precision)
    query_gradient = query_gradient + jnp.einsum('fqg,fug->fqu', head_gradients * leading_decay, forwarded_state, precision=exact_precision)
    forwarded_state = jnp.exp(log_sums[:, -1])[:, None, None] * forwarded_state + jnp.einsum(
        'nbq,nbc->nqc', rescaled_keys * trailing_decay, value_rows, precision=exact_precision)
    return forwarded_state, (blended_heads, query_gradient)


def reverse_block(forwarded_state, inputs):
    query_rows, rescaled_keys, value_rows, head_gradients, log_sums = inputs
    decay_mat = decay_table(log_sums)
    scores = jnp.einsum('htk,hsk->hts', query_rows, rescaled_keys, precision=exact_precision) * decay_mat
    back_scores = jnp.einsum('htv,hsv->hts', head_gradients, value_rows, precision=exact_precision) * decay_mat
    leading_decay = jnp.exp(log_sums)[:, :, None]
    trailing_decay = jnp.exp(log_sums[:, -1:] - log_sums)[:, :, None]
    key_portion = jnp.einsum('hts,htk->hsk', back_scores, query_rows, precision=exact_precision)
    key_portion = key_portion + jnp.einsum('lbg,ljg->lbj', value_rows * trailing_decay, forwarded_state, precision=exact_precision)
    value_portion = jnp.einsum('hts,htv->hsv', scores, head_gradients, precision=exact_precision)
    value_portion = value_portion + jnp.einsum('bea,baz->bez', rescaled_keys * trailing_decay, forwarded_state, precision=exact_precision)
    forwarded_state = jnp.exp(log_sums[:, -1])[:, None, None] * forwarded_state + jnp.einsum(
        'byj,byg->bjg', query_rows * leading_decay, head_gradients, precision=exact_precision)
    return forwarded_state, (key_portion, value_portion)


def reference(moe_input, out_grad, routes, route_weight, w_gate, w_up, w_down, w_out,
              query_heads, key_heads, value_heads, log_decay, state_in):
    routed_all = TOK_DEV * TOPK
    route_ids = routes.reshape(N_SP, routed_all)
    onehot = (route_ids[:, :, None] == jnp.arange(EXPERTS, dtype=jnp.int32)[None, None, :]).astype(jnp.int32)
    slot_index = jnp.sum(jnp.cumsum(onehot, axis=1) * onehot, axis=2) - 1
    anchor = jnp.arange(N_SP, dtype=jnp.int32)[:, None]
    row_place = (anchor * CAP + slot_index).astype(jnp.int32)
    token_id = (anchor * TOK_DEV + jnp.arange(routed_all, dtype=jnp.int32)[None, :] // TOPK).astype(jnp.int32)
    expert_rows = N_SP * CAP
    token_table = jnp.full((EXPERTS, expert_rows), -1, jnp.int32).at[route_ids, row_place].set(token_id)
    weight_table = jnp.zeros((EXPERTS, expert_rows), jnp.float32).at[route_ids, row_place].set(
        route_weight.reshape(N_SP, routed_all))
    group_width = FF // N_TP

    def one_expert(expert_items):
        token_row, weight_row, gate_w, up_w, down_w = expert_items
        filled = token_row >= 0
        picked = jnp.where(filled, token_row, 0)
        rows_in = jnp.where(filled[:, None], moe_input[picked], jnp.zeros((), jnp.bfloat16))
        scaled = stored(jnp.where(filled[:, None], weight_row[:, None] * out_grad[picked].astype(jnp.float32), 0.0))
        gate_pre = jnp.dot(rows_in, gate_w, preferred_element_type=jnp.float32)
        up_pre = jnp.dot(rows_in, up_w, preferred_element_type=jnp.float32)
        active = jax.nn.silu(gate_pre)
        hidden = stored(active * up_pre)
        hidden_back = jnp.dot(scaled, down_w.T, preferred_element_type=jnp.float32)
        down_part = jnp.dot(hidden.T, scaled, preferred_element_type=jnp.float32).astype(jnp.bfloat16)
        gate_back = stored(hidden_back * up_pre * silu_slope(gate_pre))
        up_back = stored(hidden_back * active)
        gate_part = jnp.dot(rows_in.T, gate_back, preferred_element_type=jnp.float32).astype(jnp.bfloat16)
        up_part = jnp.dot(rows_in.T, up_back, preferred_element_type=jnp.float32).astype(jnp.bfloat16)
        groups_gate = gate_back.astype(jnp.float32).reshape(expert_rows, N_TP, group_width)
        groups_up = up_back.astype(jnp.float32).reshape(expert_rows, N_TP, group_width)
        weights_gate = gate_w.astype(jnp.float32).reshape(D, N_TP, group_width)
        weights_up = up_w.astype(jnp.float32).reshape(D, N_TP, group_width)
        partial_value = jnp.einsum('rgf,dgf->grd', groups_gate, weights_gate)
        partial_value = partial_value + jnp.einsum('rgf,dgf->grd', groups_up, weights_up)
        route_back = jnp.sum(stored(partial_value).astype(jnp.float32), axis=0).astype(jnp.bfloat16)
        return gate_part, up_part, down_part, route_back

    gate_grad, up_grad, down_grad, route_back = lax.map(
        one_expert, (token_table, weight_table, w_gate, w_up, w_down))
    returned = route_back[route_ids, row_place].reshape(SEQUENCE_TOKENS, TOPK, D)
    mixed_grad = (out_grad.astype(jnp.float32) + jnp.sum(returned.astype(jnp.float32), axis=1)).astype(jnp.bfloat16)

    head_grad = stored(jnp.dot(mixed_grad, w_out, preferred_element_type=jnp.float32))
    head_gradients = head_grad.astype(jnp.float32).reshape(SEQUENCE_TOKENS, RETENTION_HEADS, DV).transpose(1, 0, 2)
    block_count = SEQUENCE_TOKENS // BLOCK
    per_span = TOK_DEV // BLOCK

    def to_blocks(array):
        return array.reshape(RETENTION_HEADS, block_count, BLOCK, array.shape[-1]).transpose(1, 0, 2, 3)

    def from_blocks(array):
        return array.transpose(1, 0, 2, 3).reshape(RETENTION_HEADS, SEQUENCE_TOKENS, array.shape[-1])

    query_rows = query_heads.astype(jnp.float32)
    rescaled_keys = key_heads.astype(jnp.float32) * DK ** -0.5
    value_rows = value_heads.astype(jnp.float32)
    log_sums = jnp.cumsum(log_decay.reshape(RETENTION_HEADS, block_count, BLOCK), axis=2).transpose(1, 0, 2)
    inputs = (to_blocks(query_rows), to_blocks(rescaled_keys), to_blocks(value_rows), to_blocks(head_gradients), log_sums)

    def forward_step(forwarded_state, block_items):
        block_index = block_items[-1]
        fresh_state = lax.dynamic_index_in_dim(state_in, block_index // per_span, axis=1, keepdims=False)
        start_state = jnp.where(block_index % per_span == 0, fresh_state, forwarded_state)
        return forward_block(start_state, block_items[:-1])

    empty_state = jnp.zeros((RETENTION_HEADS, DK, DV), jnp.float32)
    _, (blended_heads, query_gradient) = lax.scan(
        forward_step, empty_state, inputs + (jnp.arange(block_count, dtype=jnp.int32),))
    _, (key_grad, value_grad) = lax.scan(reverse_block, empty_state, inputs, reverse=True)
    mixed_flat = from_blocks(blended_heads).astype(jnp.bfloat16).transpose(1, 0, 2).reshape(SEQUENCE_TOKENS, RETENTION_HEADS * DV)
    out_proj_grad = jnp.dot(mixed_grad.T, mixed_flat, preferred_element_type=jnp.float32)
    query_gradient = from_blocks(query_gradient).astype(jnp.bfloat16)
    key_grad = (from_blocks(key_grad) * DK ** -0.5).astype(jnp.bfloat16)
    value_grad = from_blocks(value_grad).astype(jnp.bfloat16)
    return gate_grad, up_grad, down_grad, out_proj_grad, query_gradient, key_grad, value_grad
```

```python
import jax
import jax.numpy as jnp
from jax import lax
from jax.sharding import PartitionSpec as P

F32 = jnp.float32
BF16 = jnp.bfloat16


def dot(spec, a, b):
    return jnp.einsum(spec, a, b, preferred_element_type=F32)


def dispatch_table(routes, route_weight, experts, capacity):
    tok_rows = routes.shape[0]
    named = routes[:, :, None] == jnp.arange(experts, dtype=jnp.int32)[None, None, :]
    member = jnp.any(named, axis=1)
    weight = jnp.sum(jnp.where(named, route_weight[:, :, None], 0.0), axis=1)
    spot = jnp.arange(tok_rows)
    earlier = (spot[:, None] > spot[None, :]).astype(BF16)
    rank = dot("ts,se->et", earlier, member.astype(BF16)).astype(jnp.int32)
    slots = jnp.arange(capacity, dtype=jnp.int32)
    table = (rank[:, None, :] == slots[None, :, None]) & member.T[:, None, :]
    slot_weight = jnp.sum(jnp.where(table, weight.T[:, None, :], 0.0), axis=2)
    return table.astype(BF16), slot_weight


def quarter(array, axis_name, axis):
    width = array.shape[axis] // lax.axis_size(axis_name)
    return lax.dynamic_slice_in_dim(array, lax.axis_index(axis_name) * width, width, axis)


def join_features(rows):
    gathered = lax.all_gather(rows, "tp", axis=0)
    return jnp.concatenate([gathered[i] for i in range(gathered.shape[0])], axis=1)


def exchange(array, axis, step):
    count = lax.axis_size(axis)
    return lax.ppermute(array, axis, [(i, i ^ step) for i in range(count)])


def sum_features(value):
    count = lax.axis_size("tp")
    place = lax.axis_index("tp")
    width = value.shape[1] // count
    parts = [value[:, i * width : (i + 1) * width] for i in range(count)]
    step = 1
    while len(parts) > 1:
        upper = (place // step) % 2 == 1
        keep = [jnp.where(upper, b, a) for a, b in zip(parts[::2], parts[1::2])]
        send = [jnp.where(upper, a, b).astype(BF16) for a, b in zip(parts[::2], parts[1::2])]
        got = exchange(jnp.stack(send), "tp", step)
        parts = [k.astype(F32) + got[i].astype(F32) for i, k in enumerate(keep)]
        step *= 2
    return parts[0].astype(BF16)


def silu_slope(gate_pre):
    sigmoid_v = jax.nn.sigmoid(gate_pre)
    return sigmoid_v * (1.0 + gate_pre * (1.0 - sigmoid_v))


def body(
    moe_input,
    out_grad,
    routes,
    route_weight,
    w_gate,
    w_up,
    w_down,
    w_out,
    query_heads,
    key_heads,
    value_heads,
    log_decay,
    state_in,
):
    tok_rows, model_width = moe_input.shape
    picks = routes.shape[1]
    spans = lax.axis_size("sp")
    place = lax.axis_index("sp")
    experts = w_gate.shape[0] * spans
    capacity = 5 * tok_rows * picks // (4 * experts)
    head_count, _, key_size = key_heads.shape
    value_size = value_heads.shape[-1]
    scale = key_size ** (-0.5)
    wg, wu, wd = w_gate[0], w_up[0], w_down[0]

    table, slot_weight = dispatch_table(routes, route_weight, experts, capacity)
    out_grad_q = quarter(out_grad, "tp", 1)
    send_rows = dot("ect,td->ecd", table, quarter(moe_input, "tp", 1)).astype(BF16)
    send_grad = (dot("ect,td->ecd", table, out_grad_q) * slot_weight[:, :, None]).astype(BF16)
    slot_rows = experts * capacity
    rows_q = lax.all_to_all(send_rows, "sp", split_axis=0, concat_axis=0, tiled=True)
    grad_q = lax.all_to_all(send_grad, "sp", split_axis=0, concat_axis=0, tiled=True)
    rows_in = join_features(rows_q.reshape(slot_rows, -1))
    grad_in = join_features(grad_q.reshape(slot_rows, -1))

    span_sums = jnp.cumsum(log_decay, axis=1)
    spot = jnp.arange(tok_rows)
    lower = (spot[:, None] >= spot[None, :])[None]
    decay = jnp.where(
        lower, jnp.exp(jnp.where(lower, span_sums[:, :, None] - span_sums[:, None, :], 0.0)), 0.0
    )
    lead = jnp.exp(span_sums)[:, :, None]
    trail = jnp.exp(span_sums[:, -1:] - span_sums)[:, :, None]
    state = state_in[:, 0].astype(BF16)
    scores = (dot("htk,hsk->hts", query_heads, key_heads) * (decay * scale)).astype(BF16)
    mixed_heads = dot("hts,hsv->htv", scores, value_heads) + lead * dot(
        "htk,hkv->htv", query_heads, state
    )
    mixed_flat = mixed_heads.astype(BF16).transpose(1, 0, 2).reshape(tok_rows, -1)
    mixed_all = lax.all_gather(mixed_flat, "sp", axis=0, tiled=True)
    totals = lax.all_gather(span_sums[:, -1], "sp", axis=0)

    gate_pre = dot("rd,df->rf", rows_in, wg)
    up_pre = dot("rd,df->rf", rows_in, wu)
    active = jax.nn.silu(gate_pre)
    hidden = (active * up_pre).astype(BF16)
    hidden_back = dot("rd,fd->rf", grad_in, wd)
    gate_back = (hidden_back * up_pre * silu_slope(gate_pre)).astype(BF16)
    up_back = (hidden_back * active).astype(BF16)
    partial_value = dot("rf,df->rd", gate_back, wg) + dot("rf,df->rd", up_back, wu)
    part = sum_features(partial_value.astype(BF16))
    down_grad = dot("rf,rd->fd", hidden, grad_in).astype(BF16)
    gate_grad = dot("rd,rf->df", rows_in, gate_back).astype(BF16)
    up_grad = dot("rd,rf->df", rows_in, up_back).astype(BF16)

    returned = lax.all_to_all(
        part.reshape(experts, capacity, -1), "sp", split_axis=0, concat_axis=0, tiled=True
    )
    mixed_q = (out_grad_q.astype(F32) + dot("ect,ecd->td", table, returned)).astype(BF16)
    mixed_grad = lax.all_gather(mixed_q, "tp", axis=1, tiled=True)

    head_grad = jnp.dot(mixed_grad, w_out, preferred_element_type=F32).astype(BF16)
    head_grad = head_grad.reshape(tok_rows, head_count, value_size).transpose(1, 0, 2)
    lead_query = (query_heads.astype(F32) * lead).astype(BF16)
    carried = dot("htk,htv->hkv", lead_query, head_grad).astype(BF16)
    carried_all = lax.all_gather(carried.reshape(1, -1, value_size), "sp", axis=0, tiled=True)
    carried_all = carried_all.reshape(spans, head_count, key_size, value_size)
    later = jnp.arange(spans)
    between = (later[None, :] < later[:, None]) & (later[None, :] > place)
    between_sum = jnp.sum(jnp.where(between[:, :, None], totals[None], 0.0), axis=1)
    weight = jnp.where((later > place)[:, None], jnp.exp(between_sum), 0.0)
    incoming = jnp.sum(carried_all.astype(F32) * weight[:, :, None, None], axis=0).astype(BF16)

    mixed_cols = lax.all_to_all(
        mixed_grad.reshape(tok_rows, spans, -1).transpose(1, 0, 2),
        "sp",
        split_axis=0,
        concat_axis=0,
        tiled=True,
    ).reshape(spans * tok_rows, -1)
    out_proj_grad = dot("td,tc->dc", mixed_cols, mixed_all)

    back_scores = (dot("htv,hsv->hts", head_grad, value_heads) * (decay * scale)).astype(BF16)
    query_gradient = dot("hts,hsk->htk", back_scores, key_heads) + lead * dot(
        "htv,hkv->htk", head_grad, state
    )
    key_grad = dot("hts,htk->hsk", back_scores, query_heads) + (trail * scale) * dot(
        "hsv,hkv->hsk", value_heads, incoming
    )
    value_grad = dot("hts,htv->hsv", scores, head_grad) + (trail * scale) * dot(
        "hsk,hkv->hsv", key_heads, incoming
    )
    return (
        gate_grad[None],
        up_grad[None],
        down_grad[None],
        out_proj_grad,
        query_gradient.astype(BF16),
        key_grad.astype(BF16),
        value_grad.astype(BF16),
    )


def solution(mesh):
    return jax.shard_map(
        body,
        mesh=mesh,
        in_specs=(
            P("sp", None),
            P("sp", None),
            P("sp", None),
            P("sp", None),
            P("sp", None, "tp"),
            P("sp", None, "tp"),
            P("sp", "tp", None),
            P(None, "tp"),
            P("tp", "sp", None),
            P("tp", "sp", None),
            P("tp", "sp", None),
            P("tp", "sp"),
            P("tp", "sp", None, None),
        ),
        out_specs=(
            P("sp", None, "tp"),
            P("sp", None, "tp"),
            P("sp", "tp", None),
            P("sp", "tp"),
            P("tp", "sp", None),
            P("tp", "sp", None),
            P("tp", "sp", None),
        ),
        check_vma=False,
    )
```

```python
import jax
import jax.numpy as jnp
from jax import lax
from jax.experimental import pallas as pl
from jax.experimental.pallas import tpu as pltpu
from jax.sharding import PartitionSpec as P

F32 = jnp.float32
BF16 = jnp.bfloat16


def dot(spec, a, b):
    return jnp.einsum(spec, a, b, preferred_element_type=F32)


def dispatch_table(routes, route_weight, experts, capacity):
    tok_rows = routes.shape[0]
    named = routes[:, :, None] == jnp.arange(experts, dtype=jnp.int32)[None, None, :]
    member = jnp.any(named, axis=1)
    weight = jnp.sum(jnp.where(named, route_weight[:, :, None], 0.0), axis=1)
    spot = jnp.arange(tok_rows)
    earlier = (spot[:, None] > spot[None, :]).astype(BF16)
    rank = dot("ts,se->et", earlier, member.astype(BF16)).astype(jnp.int32)
    slots = jnp.arange(capacity, dtype=jnp.int32)
    table = (rank[:, None, :] == slots[None, :, None]) & member.T[:, None, :]
    slot_weight = jnp.sum(jnp.where(table, weight.T[:, None, :], 0.0), axis=2)
    return table.astype(BF16), slot_weight


def quarter(array, axis_name, axis):
    width = array.shape[axis] // lax.axis_size(axis_name)
    return lax.dynamic_slice_in_dim(array, lax.axis_index(axis_name) * width, width, axis)


MESH = pl.DeviceIdType.MESH
VMEM = pl.BlockSpec(memory_space=pltpu.VMEM)


def greet(peers):
    barrier = pltpu.get_barrier_semaphore()
    for peer in peers:
        pl.semaphore_signal(barrier, inc=1, device_id=peer, device_id_type=MESH)
    pl.semaphore_wait(barrier, len(peers))


def places():
    spans, place = lax.axis_size("sp"), lax.axis_index("sp")
    members, member = lax.axis_size("tp"), lax.axis_index("tp")
    sp_peers = [None] + [
        {"sp": lax.rem(place + k, spans), "tp": member} for k in range(1, spans)
    ]
    rows = [
        {"sp": place, "tp": lax.rem(member + 2 * j, members)} for j in range(1, members // 2)
    ]
    partner = {"sp": place, "tp": member + 1 - 2 * lax.rem(member, 2)}
    return spans, place, members, member, sp_peers, [None] + rows, partner


def remote(src, dst, send, recv, peer):
    return pltpu.make_async_remote_copy(
        src_ref=src, dst_ref=dst, send_sem=send, recv_sem=recv, device_id=peer, device_id_type=MESH
    )


def dispatch_kernel(x, out, own, sp_send, sp_recv, y_send, y_recv, c_send, c_recv):
    spans, place, members, member, sp_peers, y_peers, partner = places()
    chips = members // 2
    greet(sp_peers[1:] + y_peers[1:] + [partner])
    pending = []
    arrivals = [pltpu.make_async_copy(x.at[place], out.at[member, place], own)]
    arrivals[0].start()
    for k in range(1, spans):
        copy = remote(
            x.at[lax.rem(place + k, spans)],
            out.at[member, place],
            sp_send.at[k],
            sp_recv.at[k],
            sp_peers[k],
        )
        copy.start()
        arrivals.append(copy)

    def pass_on(j, k):
        source = lax.rem(place + spans - k, spans)
        owner = lax.rem(member + members - 2 * j, members)
        block = out.at[owner, source]
        copy = remote(block, block, c_send.at[j, k], c_recv.at[j, k], partner)
        copy.start()
        pending.append(copy)

    flights = {}
    for k in range(spans + 1):
        if k < spans:
            if k == 0:
                arrivals[0].wait()
            else:
                arrivals[k].wait_recv()
            source = lax.rem(place + spans - k, spans)
            block = out.at[member, source]
            for j in range(1, chips):
                copy = remote(block, block, y_send.at[j, k], y_recv.at[j, k], y_peers[j])
                copy.start()
                flights[j, k] = copy
            pass_on(0, k)
        if k > 0:
            for j in range(1, chips):
                flights[j, k - 1].wait_recv()
                pass_on(j, k - 1)
    for copy in pending:
        copy.wait_recv()
    for copy in arrivals[1:] + list(flights.values()) + pending:
        copy.wait_send()


def dispatch(rows):
    spans, members = lax.axis_size("sp"), lax.axis_size("tp")
    dma = pltpu.SemaphoreType.DMA
    return pl.pallas_call(
        dispatch_kernel,
        out_shape=jax.ShapeDtypeStruct((members,) + rows.shape, rows.dtype),
        in_specs=[VMEM],
        out_specs=VMEM,
        scratch_shapes=[dma, dma((spans,)), dma((spans,))]
        + [dma((members // 2, spans)) for _ in range(4)],
        cost_estimate=pl.CostEstimate(flops=0, bytes_accessed=60 << 20, transcendentals=0),
        compiler_params=pltpu.CompilerParams(collective_id=0, has_side_effects=True),
    )(rows)


def swap_kernel(x, out, own, sp_send, sp_recv):
    spans, place, _, _, sp_peers, _, _ = places()
    greet(sp_peers[1:])
    mine = pltpu.make_async_copy(x.at[place], out.at[place], own)
    mine.start()
    copies = []
    for k in range(1, spans):
        copy = remote(
            x.at[lax.rem(place + k, spans)], out.at[place], sp_send.at[k], sp_recv.at[k], sp_peers[k]
        )
        copy.start()
        copies.append(copy)
    mine.wait()
    for copy in copies:
        copy.wait()


def swap(blocks):
    spans = lax.axis_size("sp")
    dma = pltpu.SemaphoreType.DMA
    return pl.pallas_call(
        swap_kernel,
        out_shape=jax.ShapeDtypeStruct(blocks.shape, blocks.dtype),
        in_specs=[VMEM],
        out_specs=VMEM,
        scratch_shapes=[dma, dma((spans,)), dma((spans,))],
        cost_estimate=pl.CostEstimate(flops=0, bytes_accessed=30 << 20, transcendentals=0),
        compiler_params=pltpu.CompilerParams(collective_id=1, has_side_effects=True),
    )(blocks)


def combine_kernel(
    x, out, from_core, pair, from_y, total, own, c_send, c_recv, y_send, y_recv, sp_send, sp_recv
):
    spans, place, members, member, sp_peers, y_peers, partner = places()
    chips = members // 2
    core = lax.rem(member, 2)
    chip = member // 2
    greet(sp_peers[1:] + y_peers[1:] + [partner])
    order = [lax.rem(place + k + 1, spans) for k in range(spans)]
    core_copies = {}
    for k in range(spans):
        for m in range(chips):
            copy = remote(
                x.at[2 * m + 1 - core, order[k]],
                from_core.at[m, order[k]],
                c_send.at[m, k],
                c_recv.at[m, k],
                partner,
            )
            copy.start()
            core_copies[m, k] = copy
    y_copies = {}
    sp_copies = []

    def send_y(k):
        for j in range(1, chips):
            copy = remote(
                pair.at[lax.rem(chip + j, chips), order[k]],
                from_y.at[j, order[k]],
                y_send.at[j, k],
                y_recv.at[j, k],
                y_peers[j],
            )
            copy.start()
            y_copies[j, k] = copy

    def send_sp(k):
        if k == spans - 1:
            return
        copy = remote(
            total.at[order[k]], out.at[place], sp_send.at[k], sp_recv.at[k], sp_peers[k + 1]
        )
        copy.start()
        sp_copies.append(copy)

    for k in range(spans + 1):
        if k < spans:
            for m in range(chips):
                core_copies[m, k].wait_recv()
                pair[m, order[k]] = (
                    x[2 * m + core, order[k]].astype(F32) + from_core[m, order[k]].astype(F32)
                ).astype(BF16)
        if k > 0:
            send_y(k - 1)
    for k in range(spans + 1):
        if k < spans:
            value = pair[chip, order[k]].astype(F32)
            for j in range(1, chips):
                y_copies[j, k].wait_recv()
                value = value + from_y[j, order[k]].astype(F32)
            total[order[k]] = value.astype(BF16)
        if k > 0:
            send_sp(k - 1)
    mine = pltpu.make_async_copy(total.at[place], out.at[place], own)
    mine.start()
    mine.wait()
    for copy in sp_copies:
        copy.wait_recv()
    for copy in sp_copies + list(y_copies.values()) + list(core_copies.values()):
        copy.wait_send()


def combine(parts):
    members, spans, rows, width = parts.shape
    dma = pltpu.SemaphoreType.DMA
    chips = members // 2
    slots = pltpu.VMEM((chips, spans, rows, width), BF16)
    return pl.pallas_call(
        combine_kernel,
        out_shape=jax.ShapeDtypeStruct((spans, rows, width), BF16),
        in_specs=[VMEM],
        out_specs=VMEM,
        scratch_shapes=[slots, slots, slots, pltpu.VMEM((spans, rows, width), BF16), dma]
        + [dma((chips, spans)) for _ in range(4)]
        + [dma((spans,)) for _ in range(2)],
        cost_estimate=pl.CostEstimate(flops=0, bytes_accessed=45 << 20, transcendentals=0),
        compiler_params=pltpu.CompilerParams(collective_id=2, has_side_effects=True),
    )(parts)


def silu_slope(gate_pre):
    sigmoid_v = jax.nn.sigmoid(gate_pre)
    return sigmoid_v * (1.0 + gate_pre * (1.0 - sigmoid_v))


def body(
    moe_input,
    out_grad,
    routes,
    route_weight,
    w_gate,
    w_up,
    w_down,
    w_out,
    query_heads,
    key_heads,
    value_heads,
    log_decay,
    state_in,
):
    tok_rows, model_width = moe_input.shape
    picks = routes.shape[1]
    spans = lax.axis_size("sp")
    place = lax.axis_index("sp")
    experts = w_gate.shape[0] * spans
    capacity = 5 * tok_rows * picks // (4 * experts)
    head_count, _, key_size = key_heads.shape
    value_size = value_heads.shape[-1]
    scale = key_size ** (-0.5)
    wg, wu, wd = w_gate[0], w_up[0], w_down[0]

    table, slot_weight = dispatch_table(routes, route_weight, experts, capacity)
    out_grad_q = quarter(out_grad, "tp", 1)
    send_rows = dot("ect,td->ecd", table, quarter(moe_input, "tp", 1)).astype(BF16)
    send_grad = (dot("ect,td->ecd", table, out_grad_q) * slot_weight[:, :, None]).astype(BF16)
    slot_rows = experts * capacity
    span_sums = jnp.cumsum(log_decay, axis=1)
    spot = jnp.arange(tok_rows)
    lower = (spot[:, None] >= spot[None, :])[None]
    decay = jnp.where(
        lower, jnp.exp(jnp.where(lower, span_sums[:, :, None] - span_sums[:, None, :], 0.0)), 0.0
    )
    lead = jnp.exp(span_sums)[:, :, None]
    trail = jnp.exp(span_sums[:, -1:] - span_sums)[:, :, None]
    state = state_in[:, 0].astype(BF16)
    scores = (dot("htk,hsk->hts", query_heads, key_heads) * (decay * scale)).astype(BF16)
    mixed_heads = dot("hts,hsv->htv", scores, value_heads) + lead * dot(
        "htk,hkv->htv", query_heads, state
    )
    mixed_flat = mixed_heads.astype(BF16).transpose(1, 0, 2).reshape(tok_rows, -1)
    totals = lax.all_gather(span_sums[:, -1], "sp", axis=0)

    sent = jnp.concatenate([send_rows, send_grad], axis=2)
    sent, mixed_flat, totals = lax.optimization_barrier((sent, mixed_flat, totals))
    mixed_all = lax.all_gather(mixed_flat, "sp", axis=0, tiled=True)
    arrived = dispatch(sent)
    arrived = arrived.reshape(arrived.shape[0], slot_rows, -1)
    share = send_rows.shape[2]
    rows_in = jnp.concatenate([block[:, :share] for block in arrived], axis=1)
    grad_in = jnp.concatenate([block[:, share:] for block in arrived], axis=1)

    gate_pre = dot("rd,df->rf", rows_in, wg)
    up_pre = dot("rd,df->rf", rows_in, wu)
    active = jax.nn.silu(gate_pre)
    hidden = (active * up_pre).astype(BF16)
    hidden_back = dot("rd,fd->rf", grad_in, wd)
    gate_back = (hidden_back * up_pre * silu_slope(gate_pre)).astype(BF16)
    up_back = (hidden_back * active).astype(BF16)
    partial_value = dot("rf,df->rd", gate_back, wg) + dot("rf,df->rd", up_back, wu)
    partial_value = partial_value.astype(BF16).reshape(experts, capacity, model_width)
    parts = jnp.stack(jnp.split(partial_value, model_width // share, axis=2))
    down_grad = dot("rf,rd->fd", hidden, grad_in).astype(BF16)
    gate_grad = dot("rd,rf->df", rows_in, gate_back).astype(BF16)
    up_grad = dot("rd,rf->df", rows_in, up_back).astype(BF16)

    parts, mixed_all = lax.optimization_barrier((parts, mixed_all))
    returned = combine(parts)
    mixed_q = (out_grad_q.astype(F32) + dot("ect,ecd->td", table, returned)).astype(BF16)
    mixed_grad = lax.all_gather(mixed_q, "tp", axis=1, tiled=True)

    head_grad = jnp.dot(mixed_grad, w_out, preferred_element_type=F32).astype(BF16)
    head_grad = head_grad.reshape(tok_rows, head_count, value_size).transpose(1, 0, 2)
    lead_query = (query_heads.astype(F32) * lead).astype(BF16)
    carried = dot("htk,htv->hkv", lead_query, head_grad).astype(BF16)
    carried_all = lax.all_gather(carried.reshape(1, -1, value_size), "sp", axis=0, tiled=True)
    carried_all = carried_all.reshape(spans, head_count, key_size, value_size)
    later = jnp.arange(spans)
    between = (later[None, :] < later[:, None]) & (later[None, :] > place)
    between_sum = jnp.sum(jnp.where(between[:, :, None], totals[None], 0.0), axis=1)
    weight = jnp.where((later > place)[:, None], jnp.exp(between_sum), 0.0)
    incoming = jnp.sum(carried_all.astype(F32) * weight[:, :, None, None], axis=0).astype(BF16)

    mixed_cols = swap(mixed_grad.reshape(tok_rows, spans, -1).transpose(1, 0, 2))
    mixed_cols = mixed_cols.reshape(spans * tok_rows, -1)
    out_proj_grad = dot("td,tc->dc", mixed_cols, mixed_all)

    back_scores = (dot("htv,hsv->hts", head_grad, value_heads) * (decay * scale)).astype(BF16)
    query_gradient = dot("hts,hsk->htk", back_scores, key_heads) + lead * dot(
        "htv,hkv->htk", head_grad, state
    )
    key_grad = dot("hts,htk->hsk", back_scores, query_heads) + (trail * scale) * dot(
        "hsv,hkv->hsk", value_heads, incoming
    )
    value_grad = dot("hts,htv->hsv", scores, head_grad) + (trail * scale) * dot(
        "hsk,hkv->hsv", key_heads, incoming
    )
    return (
        gate_grad[None],
        up_grad[None],
        down_grad[None],
        out_proj_grad,
        query_gradient.astype(BF16),
        key_grad.astype(BF16),
        value_grad.astype(BF16),
    )


def solution(mesh):
    return jax.shard_map(
        body,
        mesh=mesh,
        in_specs=(
            P("sp", None),
            P("sp", None),
            P("sp", None),
            P("sp", None),
            P("sp", None, "tp"),
            P("sp", None, "tp"),
            P("sp", "tp", None),
            P(None, "tp"),
            P("tp", "sp", None),
            P("tp", "sp", None),
            P("tp", "sp", None),
            P("tp", "sp"),
            P("tp", "sp", None, None),
        ),
        out_specs=(
            P("sp", None, "tp"),
            P("sp", None, "tp"),
            P("sp", "tp", None),
            P("sp", "tp"),
            P("tp", "sp", None),
            P("tp", "sp", None),
            P("tp", "sp", None),
        ),
        check_vma=False,
    )
```
